32 devices in a mesh: sp: 8 (over z, x), dp: 4 (over y, core).
Axes of the slice: x: 2, y: 2, z: 4, core: 2. Of those that a mesh axis runs over, the one named last changes fastest.
Arguments:
- normed_input: bfloat16 [2560, 2048], P('sp'), may hold values from -6 to 6
- out_grad: bfloat16 [2560, 2048], P('sp'), may hold values from -6 to 6
- value_weight: bfloat16 [2048, 1024], P(None, 'dp'), may hold values from -0.125 to 0.125
- gate_weight: bfloat16 [2048, 1024], P(None, 'dp'), may hold values from -0.125 to 0.125
- down_weight: bfloat16 [1024, 2048], P('dp'), may hold values from -0.1875 to 0.1875
- conv_kernel: float32 [31, 1024], P(None, 'dp'), may hold values from -5 to 5
- conv_bias: float32 [1024], P('dp'), may hold values from -3 to 3
- norm_gain: float32 [1024], P('dp'), may hold values from 0.1 to 1.9
- norm_shift: float32 [1024], P('dp'), may hold values from -3 to 3
Outputs:
- input_grad: bfloat16 [2560, 2048], P('sp')
- value_grad: float32 [2048, 1024], P('sp', 'dp')
- gate_grad: float32 [2048, 1024], P('sp', 'dp')
- down_grad: float32 [1024, 2048], P('dp', 'sp')
- kernel_grad: float32 [31, 1024], P(None, 'dp')
- bias_grad: float32 [1024], P('dp')
- gain_grad: float32 [1024], P('dp')
- shift_grad: float32 [1024], P('dp')
The draws below stay inside these ranges and needn't reach their ends.
All inputs are finite; a program needn't handle non-finite values.
Results may differ from the reference program's by a relative error of at most 0.006.
Values may be sent and summed in bfloat16 or wider, within the bound.
No kernel may reach another device: no remote copies, remote signals or barrier semaphores. Data moves between devices by JAX's collectives and lax.ppermute only.
A program may use at most 64 MiB of HBM per device.

```python
import math
import jax
import jax.numpy as jnp
from jax import lax

D = 2048
C = 1024
KW = 31
TOKENS = 2560


def draw_conv_kernel(key, part):
    first, second = jax.random.split(jax.random.fold_in(key, 11))
    place = jnp.arange(C, dtype=jnp.float32) / C
    jitter = jax.random.uniform(first, (C,), jnp.float32, -0.25, 0.25)
    scale = jnp.exp(jnp.log(0.5) + jnp.log(10.0) * place + jitter)
    base = jnp.clip(jax.random.normal(second, (KW, C), jnp.float32), -4.0, 4.0)
    return base * scale[None, :] / math.sqrt(KW)


def draw_conv_bias(key, part):
    noise_key = jax.random.fold_in(key, 23)
    place = jnp.arange(C, dtype=jnp.float32) / C
    noise = jnp.clip(jax.random.normal(noise_key, (C,), jnp.float32), -4.0, 4.0)
    return -0.8 + 2.0 * place + 0.4 * noise


def strengthened(array, key, source, target, blocks, factor):
    def block_of(dim):
        return (jnp.arange(array.shape[dim]) // (array.shape[dim] // blocks)).reshape((-1,) + (1,) * (array.ndim - 1 - dim))

    one_side = jax.random.permutation(key, blocks)[block_of(target)]
    second = (block_of(target) + blocks // 2) % blocks
    return jnp.where((block_of(source) == one_side) | (block_of(source) == second), factor * array, array)


def steps_of(key, shape, shards, least, high):
    gain, own = 1.0, jax.random.fold_in(key, 6)
    for axis_at, blocks in shards:
        draws = jnp.exp(jax.random.uniform(jax.random.fold_in(own, axis_at), (blocks,), jnp.float32, least / len(shards), high / len(shards)))
        gain = gain * jnp.repeat(draws, shape[axis_at] // blocks).reshape([-1 if axis == axis_at else 1 for axis in range(len(shape))])
    return gain


def bell_draw(rng, shape, scale, bound, cuts=(), kind=jnp.bfloat16):
    values = scale * jax.random.normal(rng, shape, jnp.float32)
    if cuts:
        values = values * steps_of(rng, shape, cuts, -0.22, 0.18)
    return jnp.clip(values, -bound, bound).astype(kind)


def heavy_noise(own_key, extent, scale, most, pieces, heavy, kind=jnp.bfloat16):
    values = scale * jax.random.normal(own_key, extent, jnp.float32)
    if pieces:
        values = values * steps_of(own_key, extent, pieces, -0.22, 0.18)
    return jnp.clip(strengthened(values, jax.random.fold_in(own_key, 3), *heavy), -most, most).astype(kind)


def setup_inputs(seed: int = 0) -> dict:
    keys = jax.random.split(jax.random.key(seed), 10)
    normed_input = heavy_noise(keys[0], (TOKENS, D), 1.0, 6.0, ((0, 8),), (0, 1, 8, 2.0))
    out_grad = heavy_noise(keys[1], (TOKENS, D), 1.0, 6.0, ((0, 8),), (0, 1, 8, 2.0))
    value_weight = bell_draw(keys[2], (D, C), D ** -0.5, 0.125, ((1, 4),))
    gate_weight = bell_draw(keys[3], (D, C), D ** -0.5, 0.125, ((1, 4),))
    down_weight = bell_draw(keys[4], (C, D), C ** -0.5, 0.1875, ((0, 4),))
    conv_kernel = draw_conv_kernel(jax.random.fold_in(keys[9], 71), 0)
    conv_bias = draw_conv_bias(jax.random.fold_in(keys[9], 71), 0)
    norm_gain = jnp.clip(1.0 + 0.18 * jax.random.normal(keys[7], (C,), jnp.float32), 0.1, 1.9)
    norm_shift = bell_draw(keys[8], (C,), 0.5, 3.0, ((0, 4),), jnp.float32)
    return {"normed_input": normed_input, "out_grad": out_grad, "value_weight": value_weight, "gate_weight": gate_weight, "down_weight": down_weight, "conv_kernel": conv_kernel, "conv_bias": conv_bias, "norm_gain": norm_gain, "norm_shift": norm_shift}


EPS = 1e-05

def reference(normed_input, out_grad, value_weight, gate_weight, down_weight, conv_kernel, conv_bias, norm_gain, norm_shift):
    reach = KW // 2
    ratio = 1.0 / math.sqrt(TOKENS)
    value_b = jnp.dot(normed_input, value_weight, preferred_element_type=jnp.float32).astype(jnp.bfloat16)
    gate_b = jnp.dot(normed_input, gate_weight, preferred_element_type=jnp.float32).astype(jnp.bfloat16)
    value = lax.optimization_barrier(value_b).astype(jnp.float32)
    gate = lax.optimization_barrier(gate_b).astype(jnp.float32)
    opening = jax.nn.sigmoid(gate)
    glu = value * opening
    padded = jnp.pad(glu, ((reach, reach), (0, 0)))
    mixed = jnp.zeros_like(glu) + conv_bias[None, :]
    for tap in range(KW):
        mixed = mixed + conv_kernel[tap][None, :] * padded[tap:tap + TOKENS]
    mean = lax.optimization_barrier(jnp.mean(mixed, axis=1, keepdims=True))
    spread = lax.optimization_barrier(jnp.mean((mixed - mean) * (mixed - mean), axis=1, keepdims=True))
    inv_std = lax.rsqrt(spread + EPS)
    centred = (mixed - mean) * inv_std
    normed = centred * norm_gain[None, :] + norm_shift[None, :]
    sig = jax.nn.sigmoid(normed)
    activated = (normed * sig).astype(jnp.bfloat16)
    d_act = jnp.dot(out_grad, down_weight.T, preferred_element_type=jnp.float32)
    d_normed = d_act * sig * (1.0 + normed * (1.0 - sig))
    d_centred = d_normed * norm_gain[None, :]
    first = lax.optimization_barrier(jnp.mean(d_centred, axis=1, keepdims=True))
    second = lax.optimization_barrier(jnp.mean(d_centred * centred, axis=1, keepdims=True))
    d_mixed = inv_std * (d_centred - first - centred * second)
    d_padded = jnp.pad(d_mixed, ((reach, reach), (0, 0)))
    d_glu = jnp.zeros_like(d_mixed)
    for tap in range(KW):
        d_glu = d_glu + conv_kernel[tap][None, :] * d_padded[2 * reach - tap:2 * reach - tap + TOKENS]
    kernel_grad = jnp.stack([lax.optimization_barrier(jnp.sum(d_mixed * padded[tap:tap + TOKENS], axis=0)) for tap in range(KW)]) * ratio
    bias_grad = lax.optimization_barrier(jnp.sum(d_mixed, axis=0)) * ratio
    gain_grad = lax.optimization_barrier(jnp.sum(d_normed * centred, axis=0)) * ratio
    shift_grad = lax.optimization_barrier(jnp.sum(d_normed, axis=0)) * ratio
    d_value = (d_glu * opening).astype(jnp.bfloat16)
    d_gate = (d_glu * value * opening * (1.0 - opening)).astype(jnp.bfloat16)
    value_grad = jnp.dot(normed_input.T, d_value, preferred_element_type=jnp.float32) * ratio
    gate_grad = jnp.dot(normed_input.T, d_gate, preferred_element_type=jnp.float32) * ratio
    down_grad = jnp.dot(activated.T, out_grad, preferred_element_type=jnp.float32) * ratio
    input_grad = (jnp.dot(d_value, value_weight.T, preferred_element_type=jnp.float32) + jnp.dot(d_gate, gate_weight.T, preferred_element_type=jnp.float32)).astype(jnp.bfloat16)
    return (input_grad, value_grad, gate_grad, down_grad, kernel_grad, bias_grad, gain_grad, shift_grad)
```

```python
import math

import jax
import jax.numpy as jnp
from jax import lax
from jax.sharding import PartitionSpec as P


EPS = 1e-05


def dot(a, b, ca, cb):
    return lax.dot_general(a, b, (((ca,), (cb,)), ((), ())), preferred_element_type=jnp.float32)


def butterfly(array, axis):
    count = lax.axis_size(axis)
    bit = count // 2
    while bit:
        arrived = lax.ppermute(array, axis, [(i, i ^ bit) for i in range(count)])
        array = array + arrived
        bit //= 2
    return array


def columns_of(rows, parity):
    count = lax.axis_size("sp")
    block = rows.shape[1] // count
    return jnp.concatenate(
        [
            lax.dynamic_slice_in_dim(rows, (2 * j + parity) * block, block, axis=1)
            for j in range(count // 2)
        ],
        axis=1,
    )


def send_pair(part, ratio):
    count = lax.axis_size("sp")
    part = (part * ratio).astype(jnp.bfloat16)
    return part, lax.ppermute(part, "sp", [(i, i ^ 1) for i in range(count)])


def finish_scatter(part, got, ratio, axis):
    count = lax.axis_size("sp")
    groups = count // 2
    place = lax.axis_index("sp") // 2
    pair = part * ratio + got.astype(jnp.float32)
    block = pair.shape[axis] // groups

    def piece(which):
        return lax.dynamic_slice_in_dim(pair, which * block, block, axis=axis)

    out = piece(place)
    sent = []
    for step in range(1, groups):
        send = piece((place + step) % groups).astype(jnp.bfloat16)
        targets = [(i, ((i // 2 + step) % groups) * 2 + i % 2) for i in range(count)]
        arrived = lax.ppermute(send, "sp", targets)
        sent.append(send)
        out = out + arrived.astype(jnp.float32)
    return out, sent


def halves(own):
    side = lax.axis_index("dp") % 2
    half = own.shape[1] // 2
    keep = lax.dynamic_slice_in_dim(own, side * half, half, axis=1)
    give = lax.dynamic_slice_in_dim(own, (1 - side) * half, half, axis=1)
    return keep, give.astype(jnp.bfloat16)


def sum_over_dp(keep, give):
    count = lax.axis_size("dp")
    side = lax.axis_index("dp") % 2
    pairs = [(i, i ^ 1) for i in range(count)]
    arrived = lax.ppermute(give, "dp", pairs)
    part = keep + arrived.astype(jnp.float32)
    bit = 2
    while bit < count:
        part = part.astype(jnp.bfloat16)
        arrived = lax.ppermute(part, "dp", [(i, i ^ bit) for i in range(count)])
        part = part.astype(jnp.float32) + arrived.astype(jnp.float32)
        bit *= 2
    part = part.astype(jnp.bfloat16)
    arrived = lax.ppermute(part, "dp", pairs)
    first = jnp.where(side == 0, part, arrived)
    second = jnp.where(side == 0, arrived, part)
    return jnp.concatenate([first, second], axis=1)


def on_device(
    normed_input,
    out_grad,
    value_weight,
    gate_weight,
    down_weight,
    conv_kernel,
    conv_bias,
    norm_gain,
    norm_shift,
):
    tokens = normed_input.shape[0]
    width = conv_kernel.shape[0]
    reach = width // 2
    wide = tokens + 2 * reach
    channels = value_weight.shape[1] * lax.axis_size("dp")
    ratio = 1.0 / math.sqrt(tokens * lax.axis_size("sp"))

    value_b = dot(normed_input, value_weight, 1, 0).astype(jnp.bfloat16)
    gate_b = dot(normed_input, gate_weight, 1, 0).astype(jnp.bfloat16)
    value = lax.optimization_barrier(value_b).astype(jnp.float32)
    gate = lax.optimization_barrier(gate_b).astype(jnp.float32)
    opening = jax.nn.sigmoid(gate)
    glu = value * opening
    act_main = dot(out_grad, down_weight, 1, 1)
    forward = [(i, i + 1) for i in range(lax.axis_size("sp") - 1)]
    backward = [(target, source) for source, target in forward]
    low = jnp.concatenate([glu[tokens - 2 * reach :], act_main[tokens - reach :]], axis=0)
    high = jnp.concatenate([glu[: 2 * reach], act_main[:reach]], axis=0)
    low = lax.ppermute(low, "sp", forward)
    high = lax.ppermute(high, "sp", backward)
    glu_low, glu_high = low[: 2 * reach], high[: 2 * reach]
    padded = jnp.concatenate([glu_low, glu, glu_high], axis=0)
    mixed = jnp.zeros((wide, glu.shape[1]), jnp.float32) + conv_bias[None, :]
    for tap in range(width):
        mixed = mixed + conv_kernel[tap][None, :] * padded[tap : tap + wide]
    total, squares = lax.psum((jnp.sum(mixed, axis=1), jnp.sum(mixed * mixed, axis=1)), "dp")
    d_act = jnp.concatenate([low[2 * reach :], act_main, high[2 * reach :]], axis=0)
    mean = total / channels
    spread = jnp.maximum(squares / channels - mean * mean, 0.0)
    inv_std = lax.rsqrt(spread + EPS)
    centred = (mixed - mean[:, None]) * inv_std[:, None]
    normed = centred * norm_gain[None, :] + norm_shift[None, :]
    sig = jax.nn.sigmoid(normed)
    d_normed = d_act * sig * (1.0 + normed * (1.0 - sig))
    d_centred = d_normed * norm_gain[None, :]
    here = slice(reach, reach + tokens)
    activated = (normed * sig)[here].astype(jnp.bfloat16)
    parity = lax.axis_index("sp") % 2
    sums = (jnp.sum(d_centred, axis=1), jnp.sum(d_centred * centred, axis=1))
    down_sent, down_got = send_pair(dot(activated, columns_of(out_grad, 1 - parity), 0, 0), ratio)
    sums, _ = lax.optimization_barrier((sums, down_sent))
    first, second = lax.psum(sums, "dp")
    d_mixed = inv_std[:, None] * (
        d_centred - first[:, None] / channels - centred * (second[:, None] / channels)
    )
    d_glu = jnp.zeros_like(glu)
    for tap in range(width):
        start = 2 * reach - tap
        d_glu = d_glu + conv_kernel[tap][None, :] * d_mixed[start : start + tokens]
    d_value = (d_glu * opening).astype(jnp.bfloat16)
    d_gate = (d_glu * value * opening * (1.0 - opening)).astype(jnp.bfloat16)
    input_other = columns_of(normed_input, 1 - parity)
    value_sent, value_got = send_pair(dot(input_other, d_value, 0, 0), ratio)
    gate_sent, gate_got = send_pair(dot(input_other, d_gate, 0, 0), ratio)
    d_value, d_gate, _, _ = lax.optimization_barrier((d_value, d_gate, value_sent, gate_sent))
    own = dot(d_value, value_weight, 1, 1) + dot(d_gate, gate_weight, 1, 1)
    keep, give = halves(own)
    input_grad = sum_over_dp(keep, give)
    grad_late, activated, _ = lax.optimization_barrier((out_grad, activated, give))
    grad_own = columns_of(grad_late, parity)
    down_grad, down_sent = finish_scatter(dot(activated, grad_own, 0, 0), down_got, ratio, 1)
    input_late, d_mixed, d_normed, _ = lax.optimization_barrier(
        (normed_input, d_mixed, d_normed, down_sent)
    )
    input_own = columns_of(input_late, parity)
    value_grad, _ = finish_scatter(dot(input_own, d_value, 0, 0), value_got, ratio, 0)
    gate_grad, _ = finish_scatter(dot(input_own, d_gate, 0, 0), gate_got, ratio, 0)
    d_here = d_mixed[here]
    sums = [
        jnp.sum(d_here * padded[reach + tap : reach + tap + tokens], axis=0)
        for tap in range(width)
    ]
    sums.append(jnp.sum(d_here, axis=0))
    sums.append(jnp.sum((d_normed * centred)[here], axis=0))
    sums.append(jnp.sum(d_normed[here], axis=0))
    small = butterfly(jnp.stack(sums) * ratio, "sp")
    return (
        input_grad,
        value_grad,
        gate_grad,
        down_grad,
        small[:width],
        small[width],
        small[width + 1],
        small[width + 2],
    )


def solution(mesh):
    in_specs = (
        P("sp", None),
        P("sp", None),
        P(None, "dp"),
        P(None, "dp"),
        P("dp", None),
        P(None, "dp"),
        P("dp"),
        P("dp"),
        P("dp"),
    )
    out_specs = (
        P("sp", None),
        P("sp", "dp"),
        P("sp", "dp"),
        P("dp", "sp"),
        P(None, "dp"),
        P("dp"),
        P("dp"),
        P("dp"),
    )

    return jax.shard_map(
        on_device, mesh=mesh, in_specs=in_specs, out_specs=out_specs, check_vma=False
    )
```
